32 devices in a mesh: sp: 16 (over z, y, x), tp: 2 (over core).
Axes of the slice: x: 2, y: 2, z: 4, core: 2. Of those that a mesh axis runs over, the one named last changes fastest.
Arguments:
- resid: bfloat16 [4096, 2048], P(('sp', 'tp')), may hold values from -6 to 6
- value_in: bfloat16 [4096, 1536], P('sp', 'tp'), may hold values from -6 to 6
- gate_in: bfloat16 [4096, 1536], P('sp', 'tp'), may hold values from -8 to 8
- conv_weight: float32 [31, 1536], P(None, 'tp'), may hold values from -2.5 to 2.5
- norm_gain: float32 [1536], P('tp'), may hold values from 0.1 to 1.9
- out_weight: bfloat16 [1536, 2048], replicated, may hold values from -0.15625 to 0.15625
- ffn_gain: float32 [2048], replicated, may hold values from 0.1 to 1.9
- expert_ids: int32 [4096, 2], P(('sp', 'tp')), may hold values from 0 to 31, all different within a row; in each aligned block of 128 rows (0 to 127, 128 to 255, ...) at most 16 rows name the same one
- expert_mix: float32 [4096, 2], P(('sp', 'tp')), may hold values from 0.1 to 1
- w_gate: bfloat16 [32, 2048, 1024], P(('sp', 'tp')), may hold values from -0.125 to 0.125
- w_up: bfloat16 [32, 2048, 1024], P(('sp', 'tp')), may hold values from -0.125 to 0.125
- w_down: bfloat16 [32, 1024, 2048], P(('sp', 'tp')), may hold values from -0.1875 to 0.1875
Outputs:
- layer_out: bfloat16 [4096, 2048], P(('sp', 'tp'))
The draws below stay inside these ranges and needn't reach their ends.
Inputs may be any that keep to these rules, and one draw needn't show every extreme that they name: `expert_ids`: each row names 2 different experts; within each aligned block of 128 rows no expert is named by more than 16 rows, a bound that some block reaches.
All inputs are finite; a program needn't handle non-finite values.
Results may differ from the reference program's by a relative error of at most 0.012.
Values may be sent and summed in bfloat16 or wider, within the bound.
A program may use at most 128 MiB of HBM per device.

```python
import math
import jax
import jax.numpy as jnp
import numpy as np
from jax import lax

D = 2048
MIX = 1536
FF = 1024
CONV = 31
TOPK = 2
TOKENS = 4096
ROWS = 128
EXPERTS = 32
CAP = 16


def draw_conv_weight(key, part):
    first = jax.random.fold_in(key, 0)
    place = jnp.arange(MIX, dtype=jnp.float32) / max(MIX - 1, 1)
    scale = jnp.exp(jnp.log(4.0) * place)
    taps = jax.random.normal(first, (CONV, MIX), jnp.float32) * CONV ** (-0.5) * scale
    return jnp.clip(taps, -2.5, 2.5)


def steps_of(rng, extent, cuts, least, top_value):
    level = 1.0
    for dim, shards_of in cuts:
        steps = jax.random.uniform(jax.random.fold_in(jax.random.fold_in(rng, 6), dim), (shards_of,), jnp.float32, least / len(cuts), top_value / len(cuts))
        level = level * jnp.repeat(jnp.exp(steps), extent[dim] // shards_of).reshape((-1,) + (1,) * (len(extent) - 1 - dim))
    return level


def shared_out(stream_key, own, number, rows, number_of, top, bound, slope):
    ranking = jax.random.permutation(stream_key, number_of)
    packed, ordinary = portions_of(number_of, rows * top, bound, slope, True), portions_of(number_of, rows * top, bound, slope, False)
    places = jnp.arange(number_of)

    def named(tallies, turn):
        used = int((tallies > 0).sum())
        fixed = max(1, used // 4)
        passed = fixed + (places - fixed + turn * (used - fixed)) % max(1, number_of - fixed)
        return jnp.zeros((number_of,), jnp.int32).at[ranking[jnp.where(places < fixed, places, passed)]].set(jnp.asarray(tallies, jnp.int32))

    tallies = jnp.where(number % 4 == 0, named(packed, number // 4), named(ordinary, number - number // 4 - 1))
    mixed = jax.random.permutation(jax.random.fold_in(own, 3), number_of)
    source_of, sink = mixed[0:number_of // 2 * 2:2], mixed[1:number_of // 2 * 2:2]
    room = jnp.minimum(tallies[source_of] - 1, bound - tallies[sink]) // 2
    room = jnp.where((source_of == ranking[0]) | (sink == ranking[0]) | (tallies[sink] == 0), 0, jnp.maximum(room, 0))
    passed = jax.random.randint(jax.random.fold_in(own, 4), (number_of // 2,), 0, 1 << 20) % (room + 1)
    tallies = tallies.at[source_of].add(-passed).at[sink].add(passed)
    members = jnp.searchsorted(jnp.cumsum(tallies), jnp.arange(rows * top), side="right").astype(jnp.int32)
    listing = members.reshape(top, rows).T
    listing = listing[jax.random.permutation(jax.random.fold_in(own, 1), rows)]
    turn = jax.random.randint(jax.random.fold_in(own, 2), (rows, 1), 0, top)
    return jnp.take_along_axis(listing, (jnp.arange(top)[None, :] + turn) % top, axis=1)


def portions_of(amount, total, bound, lean, full):
    weights = [(1 << 20) // math.isqrt(grade ** lean) + 1 for grade in range(1, amount + 1)]
    largest = bound if full else min(bound, max(-(-total // amount), total * weights[0] // sum(weights)))
    least = 1 if total - largest >= amount - 1 else 0
    counts, surplus = [largest] + [least] * (amount - 1), total - largest - least * (amount - 1)
    while surplus > 0:
        candidates = [i for i in range(1, amount) if counts[i] < largest] or [i for i in range(1, amount) if counts[i] < bound]
        pool, left = sum([weights[i] for i in candidates]), surplus
        for i in candidates:
            more = min(bound - counts[i], max(1, left * weights[i] // pool), surplus)
            counts[i] = counts[i] + more
            surplus = surplus - more
    return np.array(counts)


def centred(own_key, dims, spread, limit, cuts=(), held_as=jnp.bfloat16):
    gain = steps_of(own_key, dims, cuts, -0.22, 0.18) if cuts else 1.0
    drawn = jax.random.normal(own_key, dims, jnp.float32) * spread * gain
    return jnp.minimum(jnp.maximum(drawn, -limit), limit).astype(held_as)


def setup_inputs(seed: int = 0) -> dict:
    streams_of = jax.random.split(jax.random.key(seed), 13)
    resid = centred(streams_of[0], (TOKENS, D), 1.0, 6.0, ((0, 32),))
    value_in = centred(streams_of[1], (TOKENS, MIX), 1.0, 6.0, ((0, 16), (1, 2)))
    gate_in = centred(streams_of[2], (TOKENS, MIX), 1.5, 8.0, ((0, 16), (1, 2)))
    conv_weight = draw_conv_weight(jax.random.fold_in(streams_of[12], 71), 0)
    norm_gain = jnp.clip(1.0 + 0.18 * jax.random.normal(streams_of[4], (MIX,), jnp.float32), 0.1, 1.9)
    out_weight = centred(streams_of[5], (MIX, D), MIX ** -0.5, 0.15625)
    ffn_gain = jnp.clip(1.0 + 0.18 * jax.random.normal(streams_of[6], (D,), jnp.float32), 0.1, 1.9)
    expert_ids_keys = jax.random.split(jax.random.fold_in(streams_of[7], 1), TOKENS // ROWS)
    expert_ids_turns = jax.random.permutation(jax.random.fold_in(streams_of[7], 3), TOKENS // ROWS)
    expert_ids = jax.vmap(lambda own, number: shared_out(jax.random.fold_in(streams_of[7], 2), own, number, ROWS, EXPERTS, TOPK, CAP, 2))(expert_ids_keys, expert_ids_turns).reshape((TOKENS, TOPK))
    expert_mix = jnp.clip(0.1 + 0.9 * jax.random.uniform(streams_of[8], (TOKENS, TOPK), jnp.float32) ** steps_of(streams_of[8], (TOKENS, TOPK), ((0, 32),), -0.2, 0.2), 0.1, 1.0)
    w_gate = centred(streams_of[9], (EXPERTS, D, FF), D ** -0.5, 0.125, ((0, 32),))
    w_up = centred(streams_of[10], (EXPERTS, D, FF), D ** -0.5, 0.125, ((0, 32),))
    w_down = centred(streams_of[11], (EXPERTS, FF, D), FF ** -0.5, 0.1875, ((0, 32),))
    return {"resid": resid, "value_in": value_in, "gate_in": gate_in, "conv_weight": conv_weight, "norm_gain": norm_gain, "out_weight": out_weight, "ffn_gain": ffn_gain, "expert_ids": expert_ids, "expert_mix": expert_mix, "w_gate": w_gate, "w_up": w_up, "w_down": w_down}


def reference(resid, value_in, gate_in, conv_weight, norm_gain, out_weight, ffn_gain, expert_ids, expert_mix, w_gate, w_up, w_down):
    glu = (value_in.astype(jnp.float32) * jax.nn.sigmoid(gate_in.astype(jnp.float32))).astype(jnp.bfloat16)
    reach = CONV // 2
    padded = jnp.pad(glu.astype(jnp.float32), ((reach, reach), (0, 0)))
    conv = jnp.zeros((TOKENS, MIX), jnp.float32)
    for tap in range(CONV):
        conv = conv + padded[tap:tap + TOKENS] * conv_weight[tap]
    mean = lax.optimization_barrier(jnp.mean(conv, axis=1, keepdims=True))
    msq = lax.optimization_barrier(jnp.mean(conv * conv, axis=1, keepdims=True))
    var = msq - mean * mean
    mixed = jax.nn.silu((conv - mean) * lax.rsqrt(var + 1e-05) * norm_gain).astype(jnp.bfloat16)
    proj = jnp.dot(mixed, out_weight, preferred_element_type=jnp.float32)
    stream = (resid.astype(jnp.float32) + proj).astype(jnp.bfloat16)
    wide = stream.astype(jnp.float32)
    normed = (wide * lax.rsqrt(lax.optimization_barrier(jnp.mean(wide * wide, axis=1, keepdims=True)) + 1e-06) * ffn_gain).astype(jnp.bfloat16)
    blocks = TOKENS // ROWS
    chosen = expert_ids.reshape(blocks, ROWS * TOPK)
    onehot = (chosen[:, :, None] == jnp.arange(EXPERTS, dtype=jnp.int32)[None, None, :]).astype(jnp.int32)
    rank = lax.optimization_barrier(jnp.sum(jnp.cumsum(onehot, axis=1) * onehot, axis=2)) - 1
    slot = jnp.arange(blocks, dtype=jnp.int32)[:, None] * CAP + rank
    token = jnp.arange(blocks, dtype=jnp.int32)[:, None] * ROWS + jnp.arange(ROWS * TOPK, dtype=jnp.int32)[None, :] // TOPK
    table = jnp.full((EXPERTS, blocks * CAP), TOKENS, jnp.int32)
    table = table.at[chosen.reshape(-1), slot.reshape(-1)].set(token.reshape(-1).astype(jnp.int32))
    source = jnp.concatenate([normed, jnp.zeros((1, D), jnp.bfloat16)], axis=0)

    def run(args):
        index, gate_w, up_w, down_w = args
        rows = jnp.take(source, index, axis=0)
        gate = jnp.dot(rows, gate_w, preferred_element_type=jnp.float32)
        up = jnp.dot(rows, up_w, preferred_element_type=jnp.float32)
        hidden = (jax.nn.silu(gate) * up).astype(jnp.bfloat16)
        return jnp.dot(hidden, down_w, preferred_element_type=jnp.float32).astype(jnp.bfloat16)
    results = lax.map(run, (table, w_gate, w_up, w_down))
    picked = results[chosen.reshape(-1), slot.reshape(-1)].astype(jnp.float32).reshape(TOKENS, TOPK, D)
    total = stream.astype(jnp.float32) + lax.optimization_barrier(jnp.sum(picked * expert_mix[:, :, None], axis=1))
    return total.astype(jnp.bfloat16)
```

```python
import functools
import jax
import jax.numpy as jnp
from jax import lax
from jax.experimental import pallas as pl
from jax.experimental.pallas import tpu as pltpu
from jax.sharding import PartitionSpec as P

MESH = pl.DeviceIdType.MESH
BF = jnp.bfloat16
F32 = jnp.float32


def padded_2(block, sides, width):
    for axis, dim in sides:
        count = lax.axis_size(axis)
        forward = [(i, i + 1) for i in range(count - 1)]
        backward = [(target, source) for source, target in forward]
        low = lax.ppermute(
            lax.slice_in_dim(block, block.shape[dim] - width, None, axis=dim), axis, forward
        )
        high = lax.ppermute(lax.slice_in_dim(block, 0, width, axis=dim), axis, backward)
        block = jnp.concatenate([low, block, high], axis=dim)
    return block


def experts_kernel(
    sp_count, tp_count, cap, chunks,
    tok, stream, info, wg_h, wu_h, wd_h, out,
    wg, wu, wd, ptok, pinfo, pack, rx, hid, ys, yr, ps, pr, acc,
    w_sem, pi_sem, pt_sem, d_send, d_recv, r_send, r_recv, pp_sem,
):
    half = sp_count // 2
    n_dev = half * tp_count
    rows, width = tok.shape
    dc = width // chunks
    slots = n_dev * cap
    me_sp = lax.axis_index("sp")
    me_tp = lax.axis_index("tp")
    local = lax.rem(me_sp, half)
    base = me_sp - local
    mine = local * tp_count + me_tp
    partner = (lax.rem(me_sp + half, sp_count), me_tp)

    def peer(i):
        n = lax.rem(mine + i, n_dev)
        return n, (base + n // tp_count, lax.rem(n, tp_count))

    weights = [
        pltpu.make_async_copy(h, v, w_sem.at[k])
        for k, (h, v) in enumerate(((wg_h, wg), (wu_h, wu), (wd_h, wd)))
    ]
    for w in weights:
        w.start()

    barrier = pltpu.get_barrier_semaphore()

    @pl.loop(1, n_dev)
    def _(i):
        pl.semaphore_signal(barrier, inc=1, device_id=peer(i)[1], device_id_type=MESH)

    pl.semaphore_signal(barrier, inc=1, device_id=partner, device_id_type=MESH)
    pl.semaphore_wait(barrier, n_dev)

    def remote(src, dst, send, recv, where):
        return pltpu.make_async_remote_copy(
            src_ref=src, dst_ref=dst, send_sem=send, recv_sem=recv,
            device_id=where, device_id_type=MESH,
        )

    info_copy = remote(info, pinfo, pi_sem.at[0], pi_sem.at[1], partner)
    info_copy.start()
    tok_copies = [
        remote(tok.at[:, c * dc : (c + 1) * dc], ptok.at[c], pt_sem.at[0, c], pt_sem.at[1, c], partner)
        for c in range(chunks)
    ]
    for t in tok_copies:
        t.start()

    def slot_match(ref):
        ids = lax.broadcasted_iota(jnp.int32, (slots, rows), 0) + base * (tp_count * cap)
        ids = ids.astype(F32)
        return ids == ref[0:1, :], ids == ref[1:2, :]

    def exchange(src, dst, send, recv, s, c):
        @pl.loop(1, n_dev)
        def _(i):
            n, where = peer(i)
            remote(src.at[s, c, n], dst.at[s, c, mine], send.at[s, c], recv.at[s, c], where).start()

        pltpu.make_async_copy(src.at[s, c, mine], dst.at[s, c, mine], recv.at[s, c]).start()

    def all_in(dst, recv, s, c):
        pltpu.make_async_copy(dst.at[s, c], dst.at[s, c], recv.at[s, c]).wait()

    def all_out(src, send, s, c):
        part = src.at[s, c, pl.ds(0, n_dev - 1)]
        pltpu.make_async_copy(part, part, send.at[s, c]).wait()

    def pack_send(s, c, match, block):
        picked = jnp.dot(match, block, preferred_element_type=F32)
        pack[s, c] = picked.astype(BF).reshape(n_dev, cap, dc)
        exchange(pack, rx, d_send, d_recv, s, c)

    def one_hot(ref):
        a, b = slot_match(ref)
        return jnp.where(a | b, 1.0, 0.0).astype(BF)

    own = one_hot(info)
    for c in range(chunks):
        pack_send(0, c, own, tok[:, c * dc : (c + 1) * dc])
    info_copy.wait_recv()
    other = one_hot(pinfo)

    def run_experts(s):
        for c in range(chunks):
            all_in(rx, d_recv, s, c)
        ff = wg.shape[1]
        tile = min(256, ff)

        @pl.loop(0, ff // tile)
        def _(f):
            cols = pl.ds(pl.multiple_of(f * tile, tile), tile)
            gate = jnp.zeros((slots, tile), F32)
            up = jnp.zeros((slots, tile), F32)
            for c in range(chunks):
                x = rx[s, c].reshape(slots, dc)
                gate = gate + jnp.dot(x, wg[c * dc : (c + 1) * dc, cols], preferred_element_type=F32)
                up = up + jnp.dot(x, wu[c * dc : (c + 1) * dc, cols], preferred_element_type=F32)
            hid[:, cols] = (gate * jax.nn.sigmoid(gate) * up).astype(BF)

        for c in range(chunks):
            y = jnp.dot(hid[...], wd[:, c * dc : (c + 1) * dc], preferred_element_type=F32)
            ys[s, c] = y.astype(BF).reshape(n_dev, cap, dc)
            exchange(ys, yr, r_send, r_recv, s, c)

    tok_copies[0].wait_recv()
    pack_send(1, 0, other, ptok[0])
    for w in weights:
        w.wait()
    run_experts(0)
    for c in range(1, chunks):
        tok_copies[c].wait_recv()
        pack_send(1, c, other, ptok[c])
    run_experts(1)

    def mix_matrix(ref):
        a, b = slot_match(ref)
        full = jnp.where(a, ref[2:3, :], 0.0) + jnp.where(b, ref[3:4, :], 0.0)
        high = full.astype(BF)
        return high, (full - high.astype(F32)).astype(BF)

    def combine(s, c, mats):
        y = yr[s, c].reshape(slots, dc)
        dims = (((0,), (0,)), ((), ()))
        return sum(lax.dot_general(m, y, dims, preferred_element_type=F32) for m in mats)

    own_mix = mix_matrix(info)
    for c in range(chunks):
        all_in(yr, r_recv, 0, c)
        acc[:, c * dc : (c + 1) * dc] = stream[:, c * dc : (c + 1) * dc].astype(F32) + combine(0, c, own_mix)
    other_mix = mix_matrix(pinfo)
    parts = []
    for c in range(chunks):
        all_in(yr, r_recv, 1, c)
        ps[c] = combine(1, c, other_mix).astype(BF)
        copy = remote(ps.at[c], pr.at[c], pp_sem.at[0, c], pp_sem.at[1, c], partner)
        copy.start()
        parts.append(copy)
    for c in range(chunks):
        parts[c].wait_recv()
        out[:, c * dc : (c + 1) * dc] = (acc[:, c * dc : (c + 1) * dc] + pr[c].astype(F32)).astype(BF)
    info_copy.wait_send()
    for c in range(chunks):
        tok_copies[c].wait_send()
        parts[c].wait_send()
        for s in range(2):
            all_out(pack, d_send, s, c)
            all_out(ys, r_send, s, c)


def experts_call(normed, stream, info, w_gate, w_up, w_down, cap):
    sp_count, tp_count = lax.axis_size("sp"), lax.axis_size("tp")
    chunks = 2
    rows, width = normed.shape
    n_dev = sp_count // 2 * tp_count
    dc = width // chunks
    ff = w_gate.shape[1]
    vm = pl.BlockSpec(memory_space=pltpu.VMEM)
    hb = pl.BlockSpec(memory_space=pl.ANY)
    blocks = pltpu.VMEM((2, chunks, n_dev, cap, dc), BF)
    dma = pltpu.SemaphoreType.DMA
    return pl.pallas_call(
        functools.partial(experts_kernel, sp_count, tp_count, cap, chunks),
        out_shape=jax.ShapeDtypeStruct((rows, width), BF),
        in_specs=[vm, vm, vm, hb, hb, hb],
        out_specs=vm,
        scratch_shapes=[
            pltpu.VMEM((width, ff), BF),
            pltpu.VMEM((width, ff), BF),
            pltpu.VMEM((ff, width), BF),
            pltpu.VMEM((chunks, rows, dc), BF),
            pltpu.VMEM(info.shape, F32),
            blocks,
            blocks,
            pltpu.VMEM((n_dev * cap, ff), BF),
            blocks,
            blocks,
            pltpu.VMEM((chunks, rows, dc), BF),
            pltpu.VMEM((chunks, rows, dc), BF),
            pltpu.VMEM((rows, width), F32),
            dma((3,)),
            dma((2,)),
            dma((2, chunks)),
            dma((2, chunks)),
            dma((2, chunks)),
            dma((2, chunks)),
            dma((2, chunks)),
            dma((2, chunks)),
        ],
        compiler_params=pltpu.CompilerParams(
            collective_id=0, has_side_effects=True, vmem_limit_bytes=56 * 1024 * 1024
        ),
        name="experts",
    )(normed, stream, info, w_gate, w_up, w_down)


def per_device(
    resid,
    value_in,
    gate_in,
    conv_weight,
    norm_gain,
    out_weight,
    ffn_gain,
    expert_ids,
    expert_mix,
    w_gate,
    w_up,
    w_down,
):
    glu = (value_in.astype(F32) * jax.nn.sigmoid(gate_in.astype(F32))).astype(BF)
    taps = conv_weight.shape[0]
    reach = taps // 2
    length = glu.shape[0]
    local_width = glu.shape[1]
    padded = padded_2(glu, (("sp", 0),), reach).astype(F32)
    conv = jnp.zeros((length, local_width), F32)
    for tap in range(taps):
        conv = conv + padded[tap : tap + length] * conv_weight[tap]
    sums = lax.psum((jnp.sum(conv, axis=1), jnp.sum(conv * conv, axis=1)), "tp")
    width = local_width * lax.axis_size("tp")
    mean = sums[0] / width
    var = sums[1] / width - mean * mean
    normed_conv = (conv - mean[:, None]) * lax.rsqrt(var + 1e-05)[:, None] * norm_gain
    mixed = jax.nn.silu(normed_conv).astype(BF)
    regrouped = lax.all_to_all(mixed, "tp", split_axis=0, concat_axis=1, tiled=True)
    proj = jnp.dot(regrouped, out_weight, preferred_element_type=F32)
    stream = (resid.astype(F32) + proj).astype(BF)
    wide = stream.astype(F32)
    normed = (
        wide * lax.rsqrt(jnp.mean(wide * wide, axis=1, keepdims=True) + 1e-06) * ffn_gain
    ).astype(BF)
    experts_all = lax.axis_size("sp") * lax.axis_size("tp")
    rows_here = stream.shape[0]
    topk = expert_ids.shape[1]
    cap = max(2, (2 * topk * rows_here + experts_all - 1) // experts_all)
    ids = expert_ids.T
    hot = (ids[:, None, :] == jnp.arange(experts_all, dtype=jnp.int32)[None, :, None]).astype(F32)
    named = jnp.sum(hot, axis=0)
    at = jnp.arange(rows_here, dtype=jnp.int32)
    before = (at[:, None] < at[None, :]).astype(BF)
    rank = jnp.dot(named.astype(BF), before, preferred_element_type=F32)
    slot = ids.astype(F32) * cap + jnp.sum(hot * rank[None], axis=1)
    info = jnp.concatenate([slot, expert_mix.T, jnp.zeros((8 - 2 * topk, rows_here), F32)], axis=0)
    return experts_call(normed, stream, info, w_gate[0], w_up[0], w_down[0], cap)


def solution(mesh):
    return jax.shard_map(
        per_device,
        mesh=mesh,
        in_specs=(
            P(("sp", "tp"), None),
            P("sp", "tp"),
            P("sp", "tp"),
            P(None, "tp"),
            P("tp"),
            P(),
            P(),
            P(("sp", "tp"), None),
            P(("sp", "tp"), None),
            P(("sp", "tp"), None, None),
            P(("sp", "tp"), None, None),
            P(("sp", "tp"), None, None),
        ),
        out_specs=P(("sp", "tp"), None),
        check_vma=False,
    )
```

```python
import functools
import jax
import jax.numpy as jnp
from jax import lax
from jax.experimental import pallas as pl
from jax.experimental.pallas import tpu as pltpu
from jax.sharding import PartitionSpec as P

MESH = pl.DeviceIdType.MESH
BF = jnp.bfloat16
F32 = jnp.float32


def layer_kernel(
    sp_count, tp_count, cap, chunks,
    resid, value_in, gate_in, taps_w, gain, ffn_gain, routes, ow_h, wg_h, wu_h, wd_h, out,
    wg, wu, wd, ptok, pinfo, pack, rx, hid, ys, yr, ps, pr, acc,
    tok, info, ow, gp, wide_in, cs, cf, gf,
    w_sem, pi_sem, pt_sem, d_send, d_recv, r_send, r_recv, pp_sem,
    h_sem, c_sem, g_sem,
):
    half = sp_count // 2
    n_dev = half * tp_count
    rows, width = resid.shape
    dc = width // chunks
    slots = n_dev * cap
    me_sp = lax.axis_index("sp")
    me_tp = lax.axis_index("tp")
    local = lax.rem(me_sp, half)
    base = me_sp - local
    mine = local * tp_count + me_tp
    partner = (lax.rem(me_sp + half, sp_count), me_tp)

    def peer(i):
        n = lax.rem(mine + i, n_dev)
        return n, (base + n // tp_count, lax.rem(n, tp_count))

    weights = [
        pltpu.make_async_copy(h, v, w_sem.at[k])
        for k, (h, v) in enumerate(((ow_h, ow), (wg_h, wg), (wu_h, wu), (wd_h, wd)))
    ]
    for w in weights:
        w.start()

    barrier = pltpu.get_barrier_semaphore()

    @pl.loop(1, n_dev)
    def _(i):
        pl.semaphore_signal(barrier, inc=1, device_id=peer(i)[1], device_id_type=MESH)

    last = sp_count - 1
    has_low, has_high = me_sp > 0, me_sp < last
    lower = (jnp.maximum(me_sp - 1, 0), me_tp)
    upper = (jnp.minimum(me_sp + 1, last), me_tp)
    twin = (me_sp, 1 - me_tp)
    pl.semaphore_signal(barrier, inc=1, device_id=partner, device_id_type=MESH)

    @pl.when(has_low)
    def _():
        pl.semaphore_signal(barrier, inc=1, device_id=lower, device_id_type=MESH)

    @pl.when(has_high)
    def _():
        pl.semaphore_signal(barrier, inc=1, device_id=upper, device_id_type=MESH)

    length, local_width = value_in.shape
    taps = taps_w.shape[0]
    reach = taps // 2
    halo = (reach + 15) // 16 * 16
    gated = value_in[...].astype(F32) * jax.nn.sigmoid(gate_in[...].astype(F32))
    gp[halo : halo + length, :] = gated.astype(BF)

    @pl.when(jnp.logical_not(has_low))
    def _():
        gp[0:halo, :] = jnp.zeros((halo, local_width), BF)

    @pl.when(jnp.logical_not(has_high))
    def _():
        gp[halo + length :, :] = jnp.zeros((halo, local_width), BF)

    pl.semaphore_wait(
        barrier, n_dev + has_low.astype(jnp.int32) + has_high.astype(jnp.int32)
    )

    def remote(src, dst, send, recv, where):
        return pltpu.make_async_remote_copy(
            src_ref=src, dst_ref=dst, send_sem=send, recv_sem=recv,
            device_id=where, device_id_type=MESH,
        )

    to_low = remote(
        gp.at[halo : 2 * halo], gp.at[halo + length : 2 * halo + length], h_sem.at[0], h_sem.at[1], lower
    )
    to_high = remote(gp.at[length : length + halo], gp.at[0:halo], h_sem.at[2], h_sem.at[3], upper)

    @pl.when(has_low)
    def _():
        to_low.start()

    @pl.when(has_high)
    def _():
        to_high.start()

    gain_copy = remote(gain, gf, g_sem.at[0], g_sem.at[1], twin)
    gain_copy.start()

    experts_all = sp_count * tp_count
    expert = lax.broadcasted_iota(jnp.int32, (experts_all, rows), 0).astype(F32)
    hot = [jnp.where(expert == routes[k : k + 1, :], 1.0, 0.0) for k in range(2)]
    earlier = lax.broadcasted_iota(jnp.int32, (rows, rows), 0)
    later = lax.broadcasted_iota(jnp.int32, (rows, rows), 1)
    before = jnp.where(earlier < later, 1.0, 0.0).astype(BF)
    rank = jnp.dot((hot[0] + hot[1]).astype(BF), before, preferred_element_type=F32)
    info[...] = routes[...]
    for k in range(2):
        info[k : k + 1, :] = routes[k : k + 1, :] * cap + jnp.sum(
            hot[k] * rank, axis=0, keepdims=True
        )
    info_copy = remote(info, pinfo, pi_sem.at[0], pi_sem.at[1], partner)
    info_copy.start()

    @pl.when(has_low)
    def _():
        to_high.wait_recv()

    @pl.when(has_high)
    def _():
        to_low.wait_recv()

    wide_in[...] = gp[...].astype(F32)
    span = rows + 2 * halo

    def convolve(first, put):
        @pl.loop(0, local_width // 128)
        def _(b):
            cols = pl.ds(pl.multiple_of(b * 128, 128), 128)
            x = wide_in[pl.ds(first, span), cols]
            total = jnp.zeros((rows, 128), F32)
            for r in range(8):
                offsets = [j for j in range(taps) if (j + halo - reach) % 8 == r]
                if not offsets:
                    continue
                shifted = x if r == 0 else pltpu.roll(x, span - r, 0)
                for j in offsets:
                    at = j + halo - reach - r
                    total = total + shifted[at : at + rows] * taps_w[j : j + 1, cols]
            put(cols, total)

    def put_out(cols, total):
        cs[:, cols] = total

    def put_own(cols, total):
        cf[0, :, cols] = total

    convolve(pl.multiple_of((1 - me_tp) * rows, rows), put_out)
    conv_copy = remote(cs, cf.at[1], c_sem.at[0], c_sem.at[1], twin)
    conv_copy.start()
    convolve(pl.multiple_of(me_tp * rows, rows), put_own)
    weights[0].wait()
    gain_copy.wait_recv()
    conv_copy.wait_recv()
    channels = local_width * tp_count
    mean = (jnp.sum(cf[0], axis=1, keepdims=True) + jnp.sum(cf[1], axis=1, keepdims=True)) / channels
    msq = (
        jnp.sum(cf[0] * cf[0], axis=1, keepdims=True) + jnp.sum(cf[1] * cf[1], axis=1, keepdims=True)
    ) / channels
    scale = lax.rsqrt(msq - mean * mean + 1e-05)

    def silu(v):
        return v * jax.nn.sigmoid(v)

    mixed = [
        silu((cf[0] - mean) * scale * gain[...]).astype(BF),
        silu((cf[1] - mean) * scale * gf[...]).astype(BF),
    ]
    whose = (me_tp, 1 - me_tp)
    square = jnp.zeros((rows, 1), F32)
    step = 512
    for c in range(width // step):
        cols = slice(c * step, (c + 1) * step)
        proj = jnp.zeros((rows, step), F32)
        for m, w in zip(mixed, whose):
            at = pl.ds(pl.multiple_of(w * local_width, local_width), local_width)
            proj = proj + jnp.dot(m, ow[at, cols], preferred_element_type=F32)
        wide = (resid[:, cols].astype(F32) + proj).astype(BF).astype(F32)
        acc[:, cols] = wide
        square = square + jnp.sum(wide * wide, axis=1, keepdims=True)
    rms = lax.rsqrt(square / width + 1e-06)
    for c in range(chunks):
        tok[c] = (
            acc[:, c * dc : (c + 1) * dc] * rms * ffn_gain[:, c * dc : (c + 1) * dc]
        ).astype(BF)

    quarter = sp_count // 4
    inner = (me_sp >= quarter) & (me_sp < sp_count - quarter)
    tok_copies = [
        remote(tok.at[c], ptok.at[c], pt_sem.at[0, c], pt_sem.at[1, c], partner)
        for c in range(chunks)
    ]

    @pl.when(inner)
    def _():
        for t in tok_copies:
            t.start()

    def slot_match(ref):
        ids = lax.broadcasted_iota(jnp.int32, (slots, rows), 0) + base * (tp_count * cap)
        ids = ids.astype(F32)
        return ids == ref[0:1, :], ids == ref[1:2, :]

    def exchange(src, dst, send, recv, s, c):
        @pl.loop(1, n_dev)
        def _(i):
            n, where = peer(i)
            remote(src.at[s, c, n], dst.at[s, c, mine], send.at[s, c], recv.at[s, c], where).start()

        pltpu.make_async_copy(src.at[s, c, mine], dst.at[s, c, mine], recv.at[s, c]).start()

    def all_in(dst, recv, s, c):
        pltpu.make_async_copy(dst.at[s, c], dst.at[s, c], recv.at[s, c]).wait()

    def all_out(src, send, s, c):
        part = src.at[s, c, pl.ds(0, n_dev - 1)]
        pltpu.make_async_copy(part, part, send.at[s, c]).wait()

    def pack_send(s, c, match, block):
        picked = jnp.dot(match, block, preferred_element_type=F32)
        pack[s, c] = picked.astype(BF).reshape(n_dev, cap, dc)
        exchange(pack, rx, d_send, d_recv, s, c)

    def one_hot(ref):
        a, b = slot_match(ref)
        return jnp.where(a | b, 1.0, 0.0).astype(BF)

    own = one_hot(info)
    for c in range(chunks):
        pack_send(0, c, own, tok[c])

    @pl.when(jnp.logical_not(inner))
    def _():
        for t in tok_copies:
            t.start()

    info_copy.wait_recv()
    other = one_hot(pinfo)

    def run_experts(s):
        for c in range(chunks):
            all_in(rx, d_recv, s, c)
        ff = wg.shape[1]
        tile = min(256, ff)

        @pl.loop(0, ff // tile)
        def _(f):
            cols = pl.ds(pl.multiple_of(f * tile, tile), tile)
            gate = jnp.zeros((slots, tile), F32)
            up = jnp.zeros((slots, tile), F32)
            for c in range(chunks):
                x = rx[s, c].reshape(slots, dc)
                gate = gate + jnp.dot(x, wg[c * dc : (c + 1) * dc, cols], preferred_element_type=F32)
                up = up + jnp.dot(x, wu[c * dc : (c + 1) * dc, cols], preferred_element_type=F32)
            hid[:, cols] = (gate * jax.nn.sigmoid(gate) * up).astype(BF)

        for c in range(chunks):
            y = jnp.dot(hid[...], wd[:, c * dc : (c + 1) * dc], preferred_element_type=F32)
            ys[s, c] = y.astype(BF).reshape(n_dev, cap, dc)
            if s == 1:
                exchange(ys, yr, r_send, r_recv, s, c)

    tok_copies[0].wait_recv()
    pack_send(1, 0, other, ptok[0])
    for w in weights[1:]:
        w.wait()
    run_experts(0)
    for c in range(1, chunks):
        tok_copies[c].wait_recv()
        pack_send(1, c, other, ptok[c])
    exchange(ys, yr, r_send, r_recv, 0, 0)
    run_experts(1)
    for c in range(1, chunks):
        exchange(ys, yr, r_send, r_recv, 0, c)

    def mix_matrix(ref):
        a, b = slot_match(ref)
        full = jnp.where(a, ref[2:3, :], 0.0) + jnp.where(b, ref[3:4, :], 0.0)
        high = full.astype(BF)
        return high, (full - high.astype(F32)).astype(BF)

    def combine(s, c, mats):
        y = yr[s, c].reshape(slots, dc)
        dims = (((0,), (0,)), ((), ()))
        return sum(lax.dot_general(m, y, dims, preferred_element_type=F32) for m in mats)

    other_mix = mix_matrix(pinfo)
    parts = []
    for c in range(chunks):
        all_in(yr, r_recv, 1, c)
        ps[c] = combine(1, c, other_mix).astype(BF)
        copy = remote(ps.at[c], pr.at[c], pp_sem.at[0, c], pp_sem.at[1, c], partner)
        copy.start()
        parts.append(copy)
    own_mix = mix_matrix(info)
    for c in range(chunks):
        all_in(yr, r_recv, 0, c)
        acc[:, c * dc : (c + 1) * dc] += combine(0, c, own_mix)
    for c in range(chunks):
        parts[c].wait_recv()
        out[:, c * dc : (c + 1) * dc] = (acc[:, c * dc : (c + 1) * dc] + pr[c].astype(F32)).astype(BF)
    info_copy.wait_send()
    gain_copy.wait_send()
    conv_copy.wait_send()

    @pl.when(has_low)
    def _():
        to_low.wait_send()

    @pl.when(has_high)
    def _():
        to_high.wait_send()

    for c in range(chunks):
        tok_copies[c].wait_send()
        parts[c].wait_send()
        for s in range(2):
            all_out(pack, d_send, s, c)
            all_out(ys, r_send, s, c)


def layer_call(resid, value_in, gate_in, taps_w, gain, ffn_gain, routes, ow, w_gate, w_up, w_down, cap):
    sp_count, tp_count = lax.axis_size("sp"), lax.axis_size("tp")
    chunks = 2
    rows, width = resid.shape
    length, local_width = value_in.shape
    halo = (taps_w.shape[0] // 2 + 15) // 16 * 16
    n_dev = sp_count // 2 * tp_count
    dc = width // chunks
    ff = w_gate.shape[1]
    vm = pl.BlockSpec(memory_space=pltpu.VMEM)
    hb = pl.BlockSpec(memory_space=pl.ANY)
    blocks = pltpu.VMEM((2, chunks, n_dev, cap, dc), BF)
    dma = pltpu.SemaphoreType.DMA
    return pl.pallas_call(
        functools.partial(layer_kernel, sp_count, tp_count, cap, chunks),
        out_shape=jax.ShapeDtypeStruct((rows, width), BF),
        in_specs=[vm] * 7 + [hb] * 4,
        out_specs=vm,
        scratch_shapes=[
            pltpu.VMEM((width, ff), BF),
            pltpu.VMEM((width, ff), BF),
            pltpu.VMEM((ff, width), BF),
            pltpu.VMEM((chunks, rows, dc), BF),
            pltpu.VMEM(routes.shape, F32),
            blocks,
            blocks,
            pltpu.VMEM((n_dev * cap, ff), BF),
            blocks,
            blocks,
            pltpu.VMEM((chunks, rows, dc), BF),
            pltpu.VMEM((chunks, rows, dc), BF),
            pltpu.VMEM((rows, width), F32),
            pltpu.VMEM((chunks, rows, dc), BF),
            pltpu.VMEM(routes.shape, F32),
            pltpu.VMEM(ow.shape, BF),
            pltpu.VMEM((length + 2 * halo, local_width), BF),
            pltpu.VMEM((length + 2 * halo, local_width), F32),
            pltpu.VMEM((rows, local_width), F32),
            pltpu.VMEM((2, rows, local_width), F32),
            pltpu.VMEM(gain.shape, F32),
            dma((4,)),
            dma((2,)),
            dma((2, chunks)),
            dma((2, chunks)),
            dma((2, chunks)),
            dma((2, chunks)),
            dma((2, chunks)),
            dma((2, chunks)),
            dma((4,)),
            dma((2,)),
            dma((2,)),
        ],
        compiler_params=pltpu.CompilerParams(
            collective_id=0, has_side_effects=True, vmem_limit_bytes=56 * 1024 * 1024
        ),
        name="layer",
    )(resid, value_in, gate_in, taps_w, gain, ffn_gain, routes, ow, w_gate, w_up, w_down)


def per_device(
    resid,
    value_in,
    gate_in,
    conv_weight,
    norm_gain,
    out_weight,
    ffn_gain,
    expert_ids,
    expert_mix,
    w_gate,
    w_up,
    w_down,
):
    experts_all = lax.axis_size("sp") * lax.axis_size("tp")
    rows_here = resid.shape[0]
    topk = expert_ids.shape[1]
    cap = max(2, (2 * topk * rows_here + experts_all - 1) // experts_all)
    routes = jnp.concatenate(
        [expert_ids.astype(F32), expert_mix, jnp.zeros((rows_here, 8 - 2 * topk), F32)], axis=1
    ).T
    return layer_call(
        resid, value_in, gate_in, conv_weight, norm_gain[None], ffn_gain[None], routes,
        out_weight, w_gate[0], w_up[0], w_down[0], cap,
    )


def solution(mesh):
    return jax.shard_map(
        per_device,
        mesh=mesh,
        in_specs=(
            P(("sp", "tp"), None),
            P("sp", "tp"),
            P("sp", "tp"),
            P(None, "tp"),
            P("tp"),
            P(),
            P(),
            P(("sp", "tp"), None),
            P(("sp", "tp"), None),
            P(("sp", "tp"), None, None),
            P(("sp", "tp"), None, None),
            P(("sp", "tp"), None, None),
        ),
        out_specs=P(("sp", "tp"), None),
        check_vma=False,
    )
```

```python
import functools
import jax
import jax.numpy as jnp
from jax import lax
from jax.experimental import pallas as pl
from jax.experimental.pallas import tpu as pltpu
from jax.sharding import PartitionSpec as P

MESH = pl.DeviceIdType.MESH
BF = jnp.bfloat16
F32 = jnp.float32


def layer_kernel(
    sp_count, tp_count, cap, chunks,
    resid, value_in, gate_in, taps_w, gain, ffn_gain, ids, mix, ow_h, wg_h, wu_h, wd_h, out,
    wg, wu, wd, ptok, pinfo, pack, rx, hid, ys, yr, ps, pr, acc,
    tok, info, ow, gp, wide_in, cs, cf, gf,
    w_sem, pi_sem, pt_sem, d_send, d_recv, r_send, r_recv, pp_sem,
    h_sem, c_sem, g_sem,
):
    half = sp_count // 2
    n_dev = half * tp_count
    rows, width = resid.shape
    dc = width // chunks
    slots = n_dev * cap
    me_sp = lax.axis_index("sp")
    me_tp = lax.axis_index("tp")
    local = lax.rem(me_sp, half)
    base = me_sp - local
    mine = local * tp_count + me_tp
    partner = (lax.rem(me_sp + half, sp_count), me_tp)

    def peer(i):
        n = lax.rem(mine + i, n_dev)
        return n, (base + n // tp_count, lax.rem(n, tp_count))

    weights = [
        pltpu.make_async_copy(h, v, w_sem.at[k])
        for k, (h, v) in enumerate(((ow_h, ow), (wg_h, wg), (wu_h, wu), (wd_h, wd)))
    ]
    for w in weights:
        w.start()

    barrier = pltpu.get_barrier_semaphore()

    @pl.loop(1, n_dev)
    def _(i):
        pl.semaphore_signal(barrier, inc=1, device_id=peer(i)[1], device_id_type=MESH)

    last = sp_count - 1
    has_low, has_high = me_sp > 0, me_sp < last
    lower = (jnp.maximum(me_sp - 1, 0), me_tp)
    upper = (jnp.minimum(me_sp + 1, last), me_tp)
    twin = (me_sp, 1 - me_tp)
    pl.semaphore_signal(barrier, inc=1, device_id=partner, device_id_type=MESH)

    @pl.when(has_low)
    def _():
        pl.semaphore_signal(barrier, inc=1, device_id=lower, device_id_type=MESH)

    @pl.when(has_high)
    def _():
        pl.semaphore_signal(barrier, inc=1, device_id=upper, device_id_type=MESH)

    length, local_width = value_in.shape
    taps = taps_w.shape[0]
    reach = taps // 2
    halo = (reach + 15) // 16 * 16
    gated = value_in[...].astype(F32) * jax.nn.sigmoid(gate_in[...].astype(F32))
    gp[halo : halo + length, :] = gated.astype(BF)

    @pl.when(jnp.logical_not(has_low))
    def _():
        gp[0:halo, :] = jnp.zeros((halo, local_width), BF)

    @pl.when(jnp.logical_not(has_high))
    def _():
        gp[halo + length :, :] = jnp.zeros((halo, local_width), BF)

    pl.semaphore_wait(
        barrier, n_dev + has_low.astype(jnp.int32) + has_high.astype(jnp.int32)
    )

    def remote(src, dst, send, recv, where):
        return pltpu.make_async_remote_copy(
            src_ref=src, dst_ref=dst, send_sem=send, recv_sem=recv,
            device_id=where, device_id_type=MESH,
        )

    to_low = remote(
        gp.at[halo : 2 * halo], gp.at[halo + length : 2 * halo + length], h_sem.at[0], h_sem.at[1], lower
    )
    to_high = remote(gp.at[length : length + halo], gp.at[0:halo], h_sem.at[2], h_sem.at[3], upper)

    @pl.when(has_low)
    def _():
        to_low.start()

    @pl.when(has_high)
    def _():
        to_high.start()

    gain_copy = remote(gain, gf, g_sem.at[0], g_sem.at[1], twin)
    gain_copy.start()

    experts_all = sp_count * tp_count
    expert = lax.broadcasted_iota(jnp.int32, (experts_all, rows), 0).astype(F32)
    named = ids[...].astype(F32)
    hot = [jnp.where(expert == named[k : k + 1, :], 1.0, 0.0) for k in range(2)]
    earlier = lax.broadcasted_iota(jnp.int32, (rows, rows), 0)
    later = lax.broadcasted_iota(jnp.int32, (rows, rows), 1)
    before = jnp.where(earlier < later, 1.0, 0.0).astype(BF)
    rank = jnp.dot((hot[0] + hot[1]).astype(BF), before, preferred_element_type=F32)
    info[2:4, :] = mix[...]
    info[4:, :] = jnp.zeros_like(info[4:, :])
    for k in range(2):
        info[k : k + 1, :] = named[k : k + 1, :] * cap + jnp.sum(
            hot[k] * rank, axis=0, keepdims=True
        )
    info_copy = remote(info, pinfo, pi_sem.at[0], pi_sem.at[1], partner)
    info_copy.start()

    @pl.when(has_low)
    def _():
        to_high.wait_recv()

    @pl.when(has_high)
    def _():
        to_low.wait_recv()

    wide_in[...] = gp[...].astype(F32)
    span = rows + 2 * halo

    def convolve(first, put):
        @pl.loop(0, local_width // 128)
        def _(b):
            cols = pl.ds(pl.multiple_of(b * 128, 128), 128)
            x = wide_in[pl.ds(first, span), cols]
            total = jnp.zeros((rows, 128), F32)
            for r in range(8):
                offsets = [j for j in range(taps) if (j + halo - reach) % 8 == r]
                if not offsets:
                    continue
                shifted = x if r == 0 else pltpu.roll(x, span - r, 0)
                for j in offsets:
                    at = j + halo - reach - r
                    total = total + shifted[at : at + rows] * taps_w[j : j + 1, cols]
            put(cols, total)

    def put_out(cols, total):
        cs[:, cols] = total

    def put_own(cols, total):
        cf[0, :, cols] = total

    convolve(pl.multiple_of((1 - me_tp) * rows, rows), put_out)
    conv_copy = remote(cs, cf.at[1], c_sem.at[0], c_sem.at[1], twin)
    conv_copy.start()
    convolve(pl.multiple_of(me_tp * rows, rows), put_own)
    weights[0].wait()
    gain_copy.wait_recv()
    conv_copy.wait_recv()
    channels = local_width * tp_count
    mean = (jnp.sum(cf[0], axis=1, keepdims=True) + jnp.sum(cf[1], axis=1, keepdims=True)) / channels
    msq = (
        jnp.sum(cf[0] * cf[0], axis=1, keepdims=True) + jnp.sum(cf[1] * cf[1], axis=1, keepdims=True)
    ) / channels
    scale = lax.rsqrt(msq - mean * mean + 1e-05)

    def silu(v):
        return v * jax.nn.sigmoid(v)

    mixed = [
        silu((cf[0] - mean) * scale * gain[...].reshape(1, local_width)).astype(BF),
        silu((cf[1] - mean) * scale * gf[...].reshape(1, local_width)).astype(BF),
    ]
    whose = (me_tp, 1 - me_tp)
    square = jnp.zeros((rows, 1), F32)
    step = 512
    for c in range(width // step):
        cols = slice(c * step, (c + 1) * step)
        proj = jnp.zeros((rows, step), F32)
        for m, w in zip(mixed, whose):
            at = pl.ds(pl.multiple_of(w * local_width, local_width), local_width)
            proj = proj + jnp.dot(m, ow[at, cols], preferred_element_type=F32)
        wide = (resid[:, cols].astype(F32) + proj).astype(BF).astype(F32)
        acc[:, cols] = wide
        square = square + jnp.sum(wide * wide, axis=1, keepdims=True)
    rms = lax.rsqrt(square / width + 1e-06)
    for c in range(chunks):
        tok[c] = (
            acc[:, c * dc : (c + 1) * dc] * rms * ffn_gain[:, c * dc : (c + 1) * dc]
        ).astype(BF)

    quarter = sp_count // 4
    inner = (me_sp >= quarter) & (me_sp < sp_count - quarter)
    tok_copies = [
        remote(tok.at[c], ptok.at[c], pt_sem.at[0, c], pt_sem.at[1, c], partner)
        for c in range(chunks)
    ]

    @pl.when(inner)
    def _():
        for t in tok_copies:
            t.start()

    def slot_match(ref):
        ids = lax.broadcasted_iota(jnp.int32, (slots, rows), 0) + base * (tp_count * cap)
        ids = ids.astype(F32)
        return ids == ref[0:1, :], ids == ref[1:2, :]

    def exchange(src, dst, send, recv, s, c):
        @pl.loop(1, n_dev)
        def _(i):
            n, where = peer(i)
            remote(src.at[s, c, n], dst.at[s, c, mine], send.at[s, c], recv.at[s, c], where).start()

        pltpu.make_async_copy(src.at[s, c, mine], dst.at[s, c, mine], recv.at[s, c]).start()

    def all_in(dst, recv, s, c):
        pltpu.make_async_copy(dst.at[s, c], dst.at[s, c], recv.at[s, c]).wait()

    def all_out(src, send, s, c):
        part = src.at[s, c, pl.ds(0, n_dev - 1)]
        pltpu.make_async_copy(part, part, send.at[s, c]).wait()

    def pack_send(s, c, match, block):
        picked = jnp.dot(match, block, preferred_element_type=F32)
        pack[s, c] = picked.astype(BF).reshape(n_dev, cap, dc)
        exchange(pack, rx, d_send, d_recv, s, c)

    def one_hot(ref):
        a, b = slot_match(ref)
        return jnp.where(a | b, 1.0, 0.0).astype(BF)

    own = one_hot(info)
    for c in range(chunks):
        pack_send(0, c, own, tok[c])

    @pl.when(jnp.logical_not(inner))
    def _():
        for t in tok_copies:
            t.start()

    info_copy.wait_recv()
    other = one_hot(pinfo)

    def run_experts(s):
        for c in range(chunks):
            all_in(rx, d_recv, s, c)
        ff = wg.shape[1]
        tile = min(256, ff)

        @pl.loop(0, ff // tile)
        def _(f):
            cols = pl.ds(pl.multiple_of(f * tile, tile), tile)
            gate = jnp.zeros((slots, tile), F32)
            up = jnp.zeros((slots, tile), F32)
            for c in range(chunks):
                x = rx[s, c].reshape(slots, dc)
                gate = gate + jnp.dot(x, wg[c * dc : (c + 1) * dc, cols], preferred_element_type=F32)
                up = up + jnp.dot(x, wu[c * dc : (c + 1) * dc, cols], preferred_element_type=F32)
            hid[:, cols] = (gate * jax.nn.sigmoid(gate) * up).astype(BF)

        for c in range(chunks):
            y = jnp.dot(hid[...], wd[:, c * dc : (c + 1) * dc], preferred_element_type=F32)
            ys[s, c] = y.astype(BF).reshape(n_dev, cap, dc)
            if s == 1:
                exchange(ys, yr, r_send, r_recv, s, c)

    early = chunks // 2
    for c in range(early):
        tok_copies[c].wait_recv()
        pack_send(1, c, other, ptok[c])
    for w in weights[1:]:
        w.wait()
    run_experts(0)
    for c in range(early, chunks):
        tok_copies[c].wait_recv()
        pack_send(1, c, other, ptok[c])
    for c in range(early):
        exchange(ys, yr, r_send, r_recv, 0, c)
    run_experts(1)
    for c in range(early, chunks):
        exchange(ys, yr, r_send, r_recv, 0, c)

    def mix_matrix(ref):
        a, b = slot_match(ref)
        full = jnp.where(a, ref[2:3, :], 0.0) + jnp.where(b, ref[3:4, :], 0.0)
        high = full.astype(BF)
        return high, (full - high.astype(F32)).astype(BF)

    def combine(s, c, mats):
        y = yr[s, c].reshape(slots, dc)
        dims = (((0,), (0,)), ((), ()))
        return sum(lax.dot_general(m, y, dims, preferred_element_type=F32) for m in mats)

    other_mix = mix_matrix(pinfo)
    parts = []
    for c in range(chunks):
        all_in(yr, r_recv, 1, c)
        ps[c] = combine(1, c, other_mix).astype(BF)
        copy = remote(ps.at[c], pr.at[c], pp_sem.at[0, c], pp_sem.at[1, c], partner)
        copy.start()
        parts.append(copy)
    own_mix = mix_matrix(info)
    for c in range(chunks):
        all_in(yr, r_recv, 0, c)
        acc[:, c * dc : (c + 1) * dc] += combine(0, c, own_mix)
    for c in range(chunks):
        parts[c].wait_recv()
        out[:, c * dc : (c + 1) * dc] = (acc[:, c * dc : (c + 1) * dc] + pr[c].astype(F32)).astype(BF)
    info_copy.wait_send()
    gain_copy.wait_send()
    conv_copy.wait_send()

    @pl.when(has_low)
    def _():
        to_low.wait_send()

    @pl.when(has_high)
    def _():
        to_high.wait_send()

    for c in range(chunks):
        tok_copies[c].wait_send()
        parts[c].wait_send()
        for s in range(2):
            all_out(pack, d_send, s, c)
            all_out(ys, r_send, s, c)


def layer_call(resid, value_in, gate_in, taps_w, gain, ffn_gain, ids, mix, ow, w_gate, w_up, w_down, cap):
    sp_count, tp_count = lax.axis_size("sp"), lax.axis_size("tp")
    chunks = 4
    rows, width = resid.shape
    length, local_width = value_in.shape
    halo = (taps_w.shape[0] // 2 + 15) // 16 * 16
    n_dev = sp_count // 2 * tp_count
    dc = width // chunks
    ff = w_gate.shape[1]
    vm = pl.BlockSpec(memory_space=pltpu.VMEM)
    hb = pl.BlockSpec(memory_space=pl.ANY)
    blocks = pltpu.VMEM((2, chunks, n_dev, cap, dc), BF)
    dma = pltpu.SemaphoreType.DMA
    return pl.pallas_call(
        functools.partial(layer_kernel, sp_count, tp_count, cap, chunks),
        out_shape=jax.ShapeDtypeStruct((rows, width), BF),
        in_specs=[vm] * 8 + [hb] * 4,
        out_specs=vm,
        scratch_shapes=[
            pltpu.VMEM((width, ff), BF),
            pltpu.VMEM((width, ff), BF),
            pltpu.VMEM((ff, width), BF),
            pltpu.VMEM((chunks, rows, dc), BF),
            pltpu.VMEM((8, rows), F32),
            blocks,
            blocks,
            pltpu.VMEM((n_dev * cap, ff), BF),
            blocks,
            blocks,
            pltpu.VMEM((chunks, rows, dc), BF),
            pltpu.VMEM((chunks, rows, dc), BF),
            pltpu.VMEM((rows, width), F32),
            pltpu.VMEM((chunks, rows, dc), BF),
            pltpu.VMEM((8, rows), F32),
            pltpu.VMEM(ow.shape, BF),
            pltpu.VMEM((length + 2 * halo, local_width), BF),
            pltpu.VMEM((length + 2 * halo, local_width), F32),
            pltpu.VMEM((rows, local_width), F32),
            pltpu.VMEM((2, rows, local_width), F32),
            pltpu.VMEM(gain.shape, F32),
            dma((4,)),
            dma((2,)),
            dma((2, chunks)),
            dma((2, chunks)),
            dma((2, chunks)),
            dma((2, chunks)),
            dma((2, chunks)),
            dma((2, chunks)),
            dma((4,)),
            dma((2,)),
            dma((2,)),
        ],
        compiler_params=pltpu.CompilerParams(
            collective_id=0, has_side_effects=True, vmem_limit_bytes=58 * 1024 * 1024
        ),
        name="layer",
    )(resid, value_in, gate_in, taps_w, gain, ffn_gain, ids, mix, ow, w_gate, w_up, w_down)


def per_device(
    resid,
    value_in,
    gate_in,
    conv_weight,
    norm_gain,
    out_weight,
    ffn_gain,
    expert_ids,
    expert_mix,
    w_gate,
    w_up,
    w_down,
):
    experts_all = lax.axis_size("sp") * lax.axis_size("tp")
    rows_here = resid.shape[0]
    topk = expert_ids.shape[1]
    cap = max(2, (2 * topk * rows_here + experts_all - 1) // experts_all)
    return layer_call(
        resid, value_in, gate_in, conv_weight, norm_gain, ffn_gain[None], expert_ids.T, expert_mix.T,
        out_weight, w_gate[0], w_up[0], w_down[0], cap,
    )


def solution(mesh):
    return jax.shard_map(
        per_device,
        mesh=mesh,
        in_specs=(
            P(("sp", "tp"), None),
            P("sp", "tp"),
            P("sp", "tp"),
            P(None, "tp"),
            P("tp"),
            P(),
            P(),
            P(("sp", "tp"), None),
            P(("sp", "tp"), None),
            P(("sp", "tp"), None, None),
            P(("sp", "tp"), None, None),
            P(("sp", "tp"), None, None),
        ),
        out_specs=P(("sp", "tp"), None),
        check_vma=False,
    )
```
